32 devices in a mesh: sp: 8 (over z, x), tp: 4 (over y, core).
Axes of the slice: x: 2, y: 2, z: 4, core: 2. Of those that a mesh axis runs over, the one named last changes fastest.
Arguments:
- resid: bfloat16 [2048, 4096], P('sp'), may hold values from -6 to 6
- pool_in: bfloat16 [2048, 1024], P('sp', 'tp'), may hold values from -6 to 6
- pool_mix: bfloat16 [4, 256, 256], P('tp'), may hold values from -0.375 to 0.375
- pool_gain: float32 [1024], P('tp'), may hold values from 0.1 to 1.9
- out_proj: bfloat16 [1024, 4096], P('tp'), may hold values from -0.1875 to 0.1875
- norm_gain: float32 [4096], replicated, may hold values from 0.1 to 1.9
- w_gate: bfloat16 [8, 4096, 1024], P('sp', None, 'tp'), may hold values from -0.09375 to 0.09375
- w_up: bfloat16 [8, 4096, 1024], P('sp', None, 'tp'), may hold values from -0.09375 to 0.09375
- w_down: bfloat16 [8, 1024, 4096], P('sp', 'tp'), may hold values from -0.1875 to 0.1875
- routes: int32 [2048, 2], P('sp'), may hold values from 0 to 7, all different within a row; in each aligned block of 64 rows (0 to 63, 64 to 127, ...) at most 32 rows name the same one
- route_weight: float32 [2048, 2], P('sp'), may hold values from 0.25 to 2.5
Outputs:
- layer_out: bfloat16 [2048, 4096], P(('sp', 'tp'))
The draws below stay inside these ranges and needn't reach their ends.
Inputs may be any that keep to these rules, and one draw needn't show every extreme that they name: `routes`: in each aligned block of 64 tokens no expert is named by more than 32 of the block's rows, and the two experts of a token differ.
All inputs are finite; a program needn't handle non-finite values.
Results may differ from the reference program's by a relative error of at most 0.015.
Values may be sent and summed in bfloat16 or wider, within the bound.
A program may use at most 128 MiB of HBM per device.

```python
import math
import jax
import jax.numpy as jnp
import numpy as np
from jax import lax

D = 4096
GROUPS = 4
PCH = 256
POOLW = 1024
FF = 1024
FF_PART = 256
TOP = 2
TOK_SUB = 64
TOKENS = 2048
EXPERTS = 8
CAP = 32
N_TP = 4


def levels(key, extent, pieces, smallest, top_value):
    def one(axis_at, blocks):
        steps = jax.random.uniform(jax.random.fold_in(jax.random.fold_in(key, 6), axis_at), (blocks,), jnp.float32, smallest / len(pieces), top_value / len(pieces))
        return jnp.repeat(jnp.exp(steps), extent[axis_at] // blocks).reshape((-1,) + (1,) * (len(extent) - axis_at - 1))

    factor_of = one(*pieces[0])
    for cut in pieces[1:]:
        factor_of = factor_of * one(*cut)
    return factor_of


def shared_out(stream_key, own, number, rows, count, top, limit, lean):
    order = jax.random.permutation(stream_key, count)
    crowded, common = portions_of(count, rows * top, limit, lean, True), portions_of(count, rows * top, limit, lean, False)
    places = jnp.arange(count)

    def named(tallies, turn):
        used = int((tallies > 0).sum())
        fixed = max(1, used // 4)
        passed = fixed + (places - fixed + turn * (used - fixed)) % max(1, count - fixed)
        return jnp.zeros((count,), jnp.int32).at[order[jnp.where(places < fixed, places, passed)]].set(jnp.asarray(tallies, jnp.int32))

    tallies = jnp.where(number % 4 == 0, named(crowded, number // 4), named(common, number - number // 4 - 1))
    mixed = jax.random.permutation(jax.random.fold_in(own, 3), count)
    giver, taker = mixed[0:count // 2 * 2:2], mixed[1:count // 2 * 2:2]
    room = jnp.minimum(tallies[giver] - 1, limit - tallies[taker]) // 2
    room = jnp.where((giver == order[0]) | (taker == order[0]) | (tallies[taker] == 0), 0, jnp.maximum(room, 0))
    passed = jax.random.randint(jax.random.fold_in(own, 4), (count // 2,), 0, 1 << 20) % (room + 1)
    tallies = tallies.at[giver].add(-passed).at[taker].add(passed)
    members = jnp.searchsorted(jnp.cumsum(tallies), jnp.arange(rows * top), side="right").astype(jnp.int32)
    listing = members.reshape(top, rows).T
    listing = listing[jax.random.permutation(jax.random.fold_in(own, 1), rows)]
    turn = jax.random.randint(jax.random.fold_in(own, 2), (rows, 1), 0, top)
    return jnp.take_along_axis(listing, (jnp.arange(top)[None, :] + turn) % top, axis=1)


def portions_of(count, total, limit, slope, full):
    portions = [(1 << 20) // math.isqrt(grade ** slope) + 1 for grade in range(1, count + 1)]
    largest = limit if full else min(limit, max(-(-total // count), total * portions[0] // sum(portions)))
    least = 1 if total - largest >= count - 1 else 0
    holding, rest = [largest] + [least] * (count - 1), total - largest - least * (count - 1)
    while rest > 0:
        candidates = [i for i in range(1, count) if holding[i] < largest] or [i for i in range(1, count) if holding[i] < limit]
        pool, left = sum([portions[i] for i in candidates]), rest
        for i in candidates:
            more = min(limit - holding[i], max(1, left * portions[i] // pool), rest)
            holding[i] = holding[i] + more
            rest = rest - more
    return np.array(holding)


def noise(own_key, shape, deviation, limit, pieces=(), held_as=jnp.bfloat16):
    array = deviation * jax.random.normal(own_key, shape, jnp.float32)
    if pieces:
        array = array * levels(own_key, shape, pieces, -0.22, 0.18)
    return jnp.clip(array, -limit, limit).astype(held_as)


def setup_inputs(seed: int = 0) -> dict:
    streams_of = jax.random.split(jax.random.key(seed), 12)
    resid = noise(streams_of[0], (TOKENS, D), 1.0, 6.0, ((0, 8),))
    pool_in = noise(streams_of[1], (TOKENS, POOLW), 1.0, 6.0, ((0, 8), (1, 4)))
    pool_mix = noise(streams_of[2], (GROUPS, PCH, PCH), PCH ** -0.5, 0.375, ((0, 4),))
    pool_gain = jnp.clip(1.0 + 0.18 * jax.random.normal(streams_of[3], (POOLW,), jnp.float32), 0.1, 1.9)
    out_proj = noise(streams_of[4], (POOLW, D), POOLW ** -0.5, 0.1875, ((0, 4),))
    norm_gain = jnp.clip(1.0 + 0.18 * jax.random.normal(streams_of[5], (D,), jnp.float32), 0.1, 1.9)
    w_gate = noise(streams_of[6], (EXPERTS, D, FF), D ** -0.5, 0.09375, ((0, 8), (2, 4)))
    w_up = noise(streams_of[7], (EXPERTS, D, FF), D ** -0.5, 0.09375, ((0, 8), (2, 4)))
    w_down = noise(streams_of[8], (EXPERTS, FF, D), FF ** -0.5, 0.1875, ((0, 8), (1, 4)))
    routes_keys = jax.random.split(jax.random.fold_in(streams_of[9], 1), TOKENS // TOK_SUB)
    routes_turns = jax.random.permutation(jax.random.fold_in(streams_of[9], 3), TOKENS // TOK_SUB)
    routes = jax.vmap(lambda own, number: shared_out(jax.random.fold_in(streams_of[9], 2), own, number, TOK_SUB, EXPERTS, TOP, CAP, 2))(routes_keys, routes_turns).reshape((TOKENS, TOP))
    route_weight = jnp.clip(jnp.exp(math.log(2.5) - 2.3025851 * jax.random.uniform(streams_of[10], (TOKENS, TOP), jnp.float32) ** levels(streams_of[10], (TOKENS, TOP), ((0, 8),), -0.2, 0.2)), 0.25, 2.5)
    return {"resid": resid, "pool_in": pool_in, "pool_mix": pool_mix, "pool_gain": pool_gain, "out_proj": out_proj, "norm_gain": norm_gain, "w_gate": w_gate, "w_up": w_up, "w_down": w_down, "routes": routes, "route_weight": route_weight}


EPS = 1e-06

def rounded(value):
    return lax.optimization_barrier(value.astype(jnp.bfloat16)).astype(jnp.float32)

def window_diff(block, width):
    row_count = block.shape[0]
    data = block.astype(jnp.float32)
    padded = jnp.concatenate([jnp.zeros((width - 1, data.shape[1]), jnp.float32), data], axis=0)
    total = jnp.zeros_like(data)
    for offset in range(width):
        total = total + padded[width - 1 - offset:width - 1 - offset + row_count]
    counted = jnp.minimum(jnp.arange(1, row_count + 1, dtype=jnp.float32), float(width))
    return (total / counted[:, None] - data).astype(jnp.bfloat16)

def reference(resid, pool_in, pool_mix, pool_gain, out_proj, norm_gain, w_gate, w_up, w_down, routes, route_weight):
    proj = jnp.zeros((TOKENS, D), jnp.float32)
    for group in range(GROUPS):
        lower = group * PCH
        diff = window_diff(pool_in[:, lower:lower + PCH], 2 ** (group + 1))
        pooled = (jnp.dot(diff, pool_mix[group], preferred_element_type=jnp.float32) * pool_gain[lower:lower + PCH]).astype(jnp.bfloat16)
        proj = proj + rounded(jnp.dot(pooled, out_proj[lower:lower + PCH], preferred_element_type=jnp.float32))
    proj = rounded(proj)
    mixed = resid.astype(jnp.float32) + proj
    scale = lax.rsqrt(lax.optimization_barrier(jnp.mean(mixed * mixed, axis=1, keepdims=True)) + EPS)
    normed = (mixed * scale * norm_gain).astype(jnp.bfloat16)
    normed_ext = jnp.concatenate([normed, jnp.zeros((1, D), jnp.bfloat16)], axis=0)
    flat_expert = routes.reshape(-1)
    flat_weight = route_weight.reshape(-1)
    flat_token = (jnp.arange(TOKENS * TOP, dtype=jnp.int32) // TOP).astype(jnp.int32)
    most = TOKENS // TOK_SUB * CAP

    def one_expert(total, expert):
        match = flat_expert == expert
        position = jnp.cumsum(match.astype(jnp.int32)) - 1
        slot = jnp.where(match, position, most).astype(jnp.int32)
        owner = jnp.full((most + 1,), TOKENS, jnp.int32).at[slot].set(flat_token)[:most]
        weight = jnp.zeros((most + 1,), jnp.float32).at[slot].set(flat_weight)[:most]
        inputs = normed_ext[owner]
        gate = jnp.dot(inputs, w_gate[expert], preferred_element_type=jnp.float32)
        upper = jnp.dot(inputs, w_up[expert], preferred_element_type=jnp.float32)
        hidden = (jax.nn.silu(gate) * upper).astype(jnp.bfloat16)
        down = w_down[expert]
        result = jnp.zeros((most, D), jnp.float32)
        for block in range(N_TP):
            lower = block * FF_PART
            result = result + rounded(jnp.dot(hidden[:, lower:lower + FF_PART], down[lower:lower + FF_PART], preferred_element_type=jnp.float32))
        total = total.at[owner].add(result * weight[:, None])
        return (total, None)
    moe, unused = lax.scan(one_expert, jnp.zeros((TOKENS + 1, D), jnp.float32), jnp.arange(EXPERTS, dtype=jnp.int32))
    return (mixed + moe[:TOKENS]).astype(jnp.bfloat16)
```

```python
import functools

import jax
import jax.numpy as jnp
from jax import lax
from jax.experimental import pallas as pl
from jax.experimental.pallas import tpu as pltpu
from jax.sharding import PartitionSpec as P

GROUPS = 4


EPS = 1e-06


def shifted(x, axis, by):
    count = lax.axis_size(axis)
    pairs = [(i, i + by) for i in range(count) if 0 <= i + by < count]
    return lax.ppermute(x, axis, pairs)


def rounded(value):
    return lax.optimization_barrier(value.astype(jnp.bfloat16)).astype(jnp.float32)


def group_diff(pool_in):
    row_count = pool_in.shape[0]
    reach = 2**GROUPS
    before = shifted(pool_in[row_count - reach :], "sp", 1)
    joined = jnp.concatenate([before, pool_in], axis=0).astype(jnp.float32)
    running = jnp.cumsum(joined, axis=0)
    width = jnp.left_shift(jnp.int32(2), lax.axis_index("tp"))
    lagged = lax.dynamic_slice_in_dim(running, reach - width, row_count, 0)
    total = running[reach:] - lagged
    place = lax.axis_index("sp") * row_count + jnp.arange(row_count, dtype=jnp.int32) + 1
    counted = jnp.minimum(place, width).astype(jnp.float32)
    return (total / counted[:, None] - joined[reach:]).astype(jnp.bfloat16)


def normalize(mixed, norm_gain):
    scale = lax.rsqrt(jnp.mean(mixed * mixed, axis=1, keepdims=True) + EPS)
    return (mixed * scale * norm_gain).astype(jnp.bfloat16)


def slot_plan(route_rows, blocks, capacity, experts):
    row_count, choose = route_rows.shape
    flat_routes = route_rows.reshape(blocks, row_count // blocks * choose)
    onehot = (
        flat_routes[:, :, None] == jnp.arange(experts, dtype=jnp.int32)[None, None, :]
    ).astype(jnp.int32)
    earlier = jnp.cumsum(onehot, axis=1) - onehot
    position = jnp.sum(earlier * onehot, axis=2)
    block_ids = jnp.arange(blocks, dtype=jnp.int32)[:, None]
    return (flat_routes * (blocks * capacity) + block_ids * capacity + position).reshape(-1)


def fill_slots(normed, targets, slot_count):
    row_count, width = normed.shape
    slots = jnp.arange(slot_count, dtype=jnp.int32)[:, None, None]
    picks = jnp.sum((targets.reshape(row_count, -1)[None] == slots).astype(jnp.bfloat16), axis=2)
    return jnp.dot(picks, normed, preferred_element_type=jnp.float32).astype(normed.dtype)


def collect(returned, targets, weights):
    row_count, choose = weights.shape
    slots = jnp.arange(returned.shape[0], dtype=jnp.int32)[None, None, :]
    chosen = targets.reshape(row_count, choose)[:, :, None] == slots
    spread = jnp.sum(jnp.where(chosen, weights[:, :, None], 0.0), axis=1)
    head = lax.reduce_precision(spread, 8, 7)
    tail = spread - head
    both = jnp.concatenate([head, tail], axis=0).astype(jnp.bfloat16)
    product = jnp.dot(both, returned, preferred_element_type=jnp.float32)
    return product[:row_count] + product[row_count:]


def expert_part(inputs, w_gate, w_up, w_down):
    gate = jnp.dot(inputs, w_gate[0], preferred_element_type=jnp.float32)
    upper = jnp.dot(inputs, w_up[0], preferred_element_type=jnp.float32)
    hidden = (jax.nn.silu(gate) * upper).astype(jnp.bfloat16)
    return jnp.dot(hidden, w_down[0], preferred_element_type=jnp.float32).astype(jnp.bfloat16)


def xor_of(a, b, n):
    total, bit = 0, 1
    while bit < n:
        total = total + ((a // bit + b // bit) % 2) * bit
        bit *= 2
    return total


def moe_kernel(
    n, slices, capacity,
    outgoing, wg_hbm, wu_hbm, wd_hbm, out,
    wg, wu, wd, rows, parts, pair_in, y_in,
    w_sem, own_sem,
    sp_send, sp_recv, fy_send, fy_recv, fa_send, fa_recv, fb_send, fb_recv,
    pp_send, pp_recv, ry_send, ry_recv, rs_send, rs_recv,
):
    me = lax.axis_index("sp")
    tp = lax.axis_index("tp")
    core, y = tp % 2, tp // 2
    mate = y * 2 + (1 - core)
    across = (1 - y) * 2 + core
    C = capacity

    def spot(c, yy):
        return pl.ds(pl.multiple_of((c * 2 + yy) * C, C), C)

    def half(c):
        return pl.ds(pl.multiple_of(c * 2 * C, 2 * C), 2 * C)

    def offset(j):
        return jnp.where(j < 2, j, n + 1 - j)

    def chunk(j):
        return xor_of(me, offset(j), n)

    def remote(src, dst, send, recv, to):
        return pltpu.make_async_remote_copy(
            src_ref=src, dst_ref=dst, send_sem=send, recv_sem=recv,
            device_id=to, device_id_type=pl.DeviceIdType.MESH,
        )

    def sp_copy(j):
        s = chunk(j)
        return remote(outgoing.at[s], rows.at[me, spot(core, y)],
                      sp_send.at[j], sp_recv.at[j], (s, tp))

    def fy_copy(j):
        s = chunk(j)
        ref = rows.at[s, spot(core, y)]
        return remote(ref, ref, fy_send.at[j], fy_recv.at[j], (me, across))

    def fa_copy(j):
        s = chunk(j)
        ref = rows.at[s, spot(core, y)]
        return remote(ref, ref, fa_send.at[j], fa_recv.at[j], (me, mate))

    def fb_copy(j):
        s = chunk(j)
        ref = rows.at[s, spot(core, 1 - y)]
        return remote(ref, ref, fb_send.at[j], fb_recv.at[j], (me, mate))

    def pp_copy(j):
        s = chunk(j)
        return remote(parts.at[s, half(1 - core)], pair_in.at[s],
                      pp_send.at[j], pp_recv.at[j], (me, mate))

    def ry_copy(j):
        s = chunk(j)
        return remote(parts.at[s, spot(core, 1 - y)], y_in.at[s],
                      ry_send.at[j], ry_recv.at[j], (me, across))

    def rs_copy(j):
        s = chunk(j)
        return remote(parts.at[s, spot(core, y)], out.at[me],
                      rs_send.at[j], rs_recv.at[j], (s, tp))

    loads = [
        pltpu.make_async_copy(wg_hbm.at[0], wg, w_sem.at[0]),
        pltpu.make_async_copy(wu_hbm.at[0], wu, w_sem.at[1]),
        pltpu.make_async_copy(wd_hbm.at[0], wd, w_sem.at[2]),
    ]
    own = pltpu.make_async_copy(outgoing.at[me], rows.at[me, spot(core, y)], own_sem)
    own.start()

    barrier = pltpu.get_barrier_semaphore()

    @pl.loop(1, n)
    def _(j):
        pl.semaphore_signal(barrier, inc=1, device_id=(xor_of(me, j, n), tp),
                               device_id_type=pl.DeviceIdType.MESH)

    for peer in (mate, across):
        pl.semaphore_signal(barrier, inc=1, device_id=(me, peer),
                               device_id_type=pl.DeviceIdType.MESH)
    pl.semaphore_wait(barrier, n + 1)

    @pl.loop(1, n)
    def _(j):
        sp_copy(j).start()

    for load in loads:
        load.start()

    def compute(s):
        x = rows[s]
        gate = jnp.dot(x, wg[...], preferred_element_type=jnp.float32)
        upper = jnp.dot(x, wu[...], preferred_element_type=jnp.float32)
        hidden = (gate * (1.0 / (1.0 + jnp.exp(-gate))) * upper).astype(jnp.bfloat16)
        width = wd.shape[1]
        tile = min(1024, width)

        @pl.loop(0, width // tile)
        def _(k):
            cols = pl.ds(pl.multiple_of(k * tile, tile), tile)
            parts[s, :, cols] = jnp.dot(
                hidden, wd[:, cols], preferred_element_type=jnp.float32
            ).astype(jnp.bfloat16)

    @pl.loop(0, n + 3)
    def _(j):
        @pl.when(j == 0)
        def _():
            own.wait()

        @pl.when((j >= 1) & (j < n))
        def _():
            sp_copy(j).wait_recv()

        @pl.when(j < n)
        def _():
            fy_copy(j).start()
            fa_copy(j).start()

        @pl.when((j >= 2) & (j < n + 2))
        def _():
            k = j - 2
            s = chunk(k)
            pp_copy(k).wait_recv()
            there = spot(core, 1 - y)
            far = pl.ds(pl.multiple_of((1 - y) * C, C), C)
            parts[s, there] = (
                parts[s, there].astype(jnp.float32) + pair_in[s, far].astype(jnp.float32)
            ).astype(jnp.bfloat16)
            ry_copy(k).start()

        @pl.when(j >= 3)
        def _():
            k = j - 3
            s = chunk(k)
            ry_copy(k).wait_recv()
            here = spot(core, y)
            near = pl.ds(pl.multiple_of(y * C, C), C)
            total = (
                parts[s, here].astype(jnp.float32)
                + pair_in[s, near].astype(jnp.float32)
                + y_in[s].astype(jnp.float32)
            ).astype(jnp.bfloat16)

            @pl.when(k == 0)
            def _():
                out[me] = total

            @pl.when(k > 0)
            def _():
                parts[s, here] = total
                rs_copy(k).start()

        @pl.when((j >= 1) & (j < n + 1))
        def _():
            k = j - 1
            fy_copy(k).wait_recv()
            fb_copy(k).start()

            @pl.when(k == 0)
            def _():
                for load in loads:
                    load.wait()

            fa_copy(k).wait_recv()
            fb_copy(k).wait_recv()
            compute(chunk(k))
            pp_copy(k).start()

    @pl.loop(0, n)
    def _(j):
        fy_copy(j).wait_send()
        fa_copy(j).wait_send()
        fb_copy(j).wait_send()
        pp_copy(j).wait_send()
        ry_copy(j).wait_send()

        @pl.when(j > 0)
        def _():
            sp_copy(j).wait_send()
            rs_copy(j).wait_send()
            rs_copy(j).wait_recv()


def moe_exchange(outgoing, w_gate, w_up, w_down, slices):
    n, capacity, width = outgoing.shape
    units = w_gate.shape[2]
    bf16 = jnp.bfloat16
    dma = pltpu.SemaphoreType.DMA
    return pl.pallas_call(
        functools.partial(moe_kernel, n, slices, capacity),
        out_shape=jax.ShapeDtypeStruct(outgoing.shape, bf16),
        in_specs=[pl.BlockSpec(memory_space=pltpu.VMEM)]
        + [pl.BlockSpec(memory_space=pl.ANY)] * 3,
        out_specs=pl.BlockSpec(memory_space=pltpu.VMEM),
        scratch_shapes=[
            pltpu.VMEM((width, units), bf16),
            pltpu.VMEM((width, units), bf16),
            pltpu.VMEM((units, width), bf16),
            pltpu.VMEM((n, slices * capacity, width), bf16),
            pltpu.VMEM((n, slices * capacity, width), bf16),
            pltpu.VMEM((n, 2 * capacity, width), bf16),
            pltpu.VMEM((n, capacity, width), bf16),
            dma((3,)),
            dma,
        ]
        + [dma((n,))] * 14,
        compiler_params=pltpu.CompilerParams(
            collective_id=1, has_side_effects=True, vmem_limit_bytes=52 * 2**20
        ),
        cost_estimate=pl.CostEstimate(
            flops=6 * n * slices * capacity * width * units,
            bytes_accessed=3 * 2 * width * units,
            transcendentals=0,
        ),
        name="moe_exchange",
    )(outgoing, w_gate, w_up, w_down)


def on_device(
    resid,
    pool_in,
    pool_mix,
    pool_gain,
    out_proj,
    norm_gain,
    w_gate,
    w_up,
    w_down,
    routes,
    route_weight,
):
    token_count, width = resid.shape
    choose = routes.shape[1]
    experts = lax.axis_size("sp")
    slices = lax.axis_size("tp")
    sub_count = token_count // slices
    capacity = max(2, 2 * sub_count * choose // experts)
    tp_index = lax.axis_index("tp")
    diff = group_diff(pool_in)
    pooled = (jnp.dot(diff, pool_mix[0], preferred_element_type=jnp.float32) * pool_gain).astype(
        jnp.bfloat16
    )
    proj = rounded(
        lax.psum_scatter(
            rounded(jnp.dot(pooled, out_proj, preferred_element_type=jnp.float32)).astype(
                jnp.bfloat16
            ),
            "tp",
            scatter_dimension=0,
            tiled=True,
        ).astype(jnp.float32)
    )
    first = tp_index * sub_count
    mixed = lax.dynamic_slice_in_dim(resid, first, sub_count, 0).astype(jnp.float32) + proj
    normed = normalize(mixed, norm_gain)
    route_rows = lax.dynamic_slice_in_dim(routes, first, sub_count, 0)
    weight_rows = lax.dynamic_slice_in_dim(route_weight, first, sub_count, 0)
    targets = slot_plan(route_rows, 1, capacity, experts)
    outgoing = fill_slots(normed, targets, experts * capacity).reshape(experts, capacity, width)
    if slices == 4 and capacity % 16 == 0 and experts & (experts - 1) == 0:
        returned = moe_exchange(outgoing, w_gate, w_up, w_down, slices)
    else:
        arrived = lax.all_to_all(outgoing, "sp", split_axis=0, concat_axis=0, tiled=True)
        block_rows = lax.all_gather(arrived, "tp", axis=0, tiled=True)
        spread = expert_part(block_rows.reshape(-1, width), w_gate, w_up, w_down).reshape(
            block_rows.shape
        )
        stacked = spread.reshape((slices,) + arrived.shape)
        received = lax.all_to_all(stacked, "tp", split_axis=0, concat_axis=0, tiled=True)
        summed = jnp.sum(received.astype(jnp.float32), axis=0)
        returned = lax.all_to_all(
            summed.astype(jnp.bfloat16), "sp", split_axis=0, concat_axis=0, tiled=True
        )
    moe = collect(returned.reshape(-1, width), targets, weight_rows)
    return (mixed + moe).astype(jnp.bfloat16)


def solution(mesh):
    in_specs = (
        P("sp", None),
        P("sp", "tp"),
        P("tp", None, None),
        P("tp"),
        P("tp", None),
        P(),
        P("sp", None, "tp"),
        P("sp", None, "tp"),
        P("sp", "tp", None),
        P("sp", None),
        P("sp", None),
    )
    out_specs = P(("sp", "tp"), None)
    return jax.shard_map(
        on_device, mesh=mesh, in_specs=in_specs, out_specs=out_specs, check_vma=False
    )
```

```python
import functools

import jax
import jax.numpy as jnp
from jax import lax
from jax.experimental import pallas as pl
from jax.experimental.pallas import tpu as pltpu
from jax.sharding import PartitionSpec as P

GROUPS = 4


EPS = 1e-06


def shifted(x, axis, by):
    count = lax.axis_size(axis)
    pairs = [(i, i + by) for i in range(count) if 0 <= i + by < count]
    return lax.ppermute(x, axis, pairs)


def rounded(value):
    return lax.optimization_barrier(value.astype(jnp.bfloat16)).astype(jnp.float32)


def group_diff(pool_in):
    row_count = pool_in.shape[0]
    reach = 2**GROUPS
    before = shifted(pool_in[row_count - reach :], "sp", 1)
    joined = jnp.concatenate([before, pool_in], axis=0).astype(jnp.float32)
    running = jnp.cumsum(joined, axis=0)
    width = jnp.left_shift(jnp.int32(2), lax.axis_index("tp"))
    lagged = lax.dynamic_slice_in_dim(running, reach - width, row_count, 0)
    total = running[reach:] - lagged
    place = lax.axis_index("sp") * row_count + jnp.arange(row_count, dtype=jnp.int32) + 1
    counted = jnp.minimum(place, width).astype(jnp.float32)
    return (total / counted[:, None] - joined[reach:]).astype(jnp.bfloat16)


def normalize(mixed, norm_gain):
    scale = lax.rsqrt(jnp.mean(mixed * mixed, axis=1, keepdims=True) + EPS)
    return (mixed * scale * norm_gain).astype(jnp.bfloat16)


def slot_plan(route_rows, blocks, capacity, experts):
    row_count, choose = route_rows.shape
    flat_routes = route_rows.reshape(blocks, row_count // blocks * choose)
    onehot = (
        flat_routes[:, :, None] == jnp.arange(experts, dtype=jnp.int32)[None, None, :]
    ).astype(jnp.int32)
    earlier = jnp.cumsum(onehot, axis=1) - onehot
    position = jnp.sum(earlier * onehot, axis=2)
    block_ids = jnp.arange(blocks, dtype=jnp.int32)[:, None]
    return (flat_routes * (blocks * capacity) + block_ids * capacity + position).reshape(-1)


def fill_slots(normed, targets, slot_count):
    row_count, width = normed.shape
    slots = jnp.arange(slot_count, dtype=jnp.int32)[:, None, None]
    picks = jnp.sum((targets.reshape(row_count, -1)[None] == slots).astype(jnp.bfloat16), axis=2)
    return jnp.dot(picks, normed, preferred_element_type=jnp.float32).astype(normed.dtype)


def collect(returned, targets, weights):
    row_count, choose = weights.shape
    slots = jnp.arange(returned.shape[0], dtype=jnp.int32)[None, None, :]
    chosen = targets.reshape(row_count, choose)[:, :, None] == slots
    spread = jnp.sum(jnp.where(chosen, weights[:, :, None], 0.0), axis=1)
    head = lax.reduce_precision(spread, 8, 7)
    tail = spread - head
    both = jnp.concatenate([head, tail], axis=0).astype(jnp.bfloat16)
    product = jnp.dot(both, returned, preferred_element_type=jnp.float32)
    return product[:row_count] + product[row_count:]


def expert_part(inputs, w_gate, w_up, w_down):
    gate = jnp.dot(inputs, w_gate[0], preferred_element_type=jnp.float32)
    upper = jnp.dot(inputs, w_up[0], preferred_element_type=jnp.float32)
    hidden = (jax.nn.silu(gate) * upper).astype(jnp.bfloat16)
    return jnp.dot(hidden, w_down[0], preferred_element_type=jnp.float32).astype(jnp.bfloat16)


def xor_of(a, b, n):
    total, bit = 0, 1
    while bit < n:
        total = total + ((a // bit + b // bit) % 2) * bit
        bit *= 2
    return total


def moe_kernel(
    n, slices, capacity,
    outgoing, wg_hbm, wu_hbm, wd_hbm, out,
    wg, wu, wd, rows, parts, pair_in, y_in,
    w_sem, own_sem,
    sp_send, sp_recv, fy_send, fy_recv, fa_send, fa_recv, fb_send, fb_recv,
    pp_send, pp_recv, ry_send, ry_recv, rs_send, rs_recv,
):
    me = lax.axis_index("sp")
    tp = lax.axis_index("tp")
    core, y = tp % 2, tp // 2
    mate = y * 2 + (1 - core)
    across = (1 - y) * 2 + core
    C = capacity

    def spot(c, yy):
        return pl.ds(pl.multiple_of((c * 2 + yy) * C, C), C)

    def half(c):
        return pl.ds(pl.multiple_of(c * 2 * C, 2 * C), 2 * C)

    def offset(j):
        return j

    def chunk(j):
        return xor_of(me, offset(j), n)

    def remote(src, dst, send, recv, to):
        return pltpu.make_async_remote_copy(
            src_ref=src, dst_ref=dst, send_sem=send, recv_sem=recv,
            device_id=to, device_id_type=pl.DeviceIdType.MESH,
        )

    def sp_copy(j):
        s = chunk(j)
        return remote(outgoing.at[s], rows.at[me, spot(core, y)],
                      sp_send.at[j], sp_recv.at[j], (s, tp))

    def fy_copy(j):
        s = chunk(j)
        ref = rows.at[s, spot(core, y)]
        return remote(ref, ref, fy_send.at[j], fy_recv.at[j], (me, across))

    def fa_copy(j):
        s = chunk(j)
        ref = rows.at[s, spot(core, y)]
        return remote(ref, ref, fa_send.at[j], fa_recv.at[j], (me, mate))

    def fb_copy(j):
        s = chunk(j)
        ref = rows.at[s, spot(core, 1 - y)]
        return remote(ref, ref, fb_send.at[j], fb_recv.at[j], (me, mate))

    def pp_copy(j):
        s = chunk(j)
        return remote(parts.at[s, half(1 - core)], pair_in.at[s],
                      pp_send.at[j], pp_recv.at[j], (me, mate))

    def ry_copy(j):
        s = chunk(j)
        return remote(parts.at[s, spot(core, 1 - y)], y_in.at[s],
                      ry_send.at[j], ry_recv.at[j], (me, across))

    def rs_copy(j):
        s = chunk(j)
        return remote(parts.at[s, spot(core, y)], out.at[me],
                      rs_send.at[j], rs_recv.at[j], (s, tp))

    loads = [
        pltpu.make_async_copy(wg_hbm.at[0], wg, w_sem.at[0]),
        pltpu.make_async_copy(wu_hbm.at[0], wu, w_sem.at[1]),
        pltpu.make_async_copy(wd_hbm.at[0], wd, w_sem.at[2]),
    ]
    own = pltpu.make_async_copy(outgoing.at[me], rows.at[me, spot(core, y)], own_sem)
    own.start()

    barrier = pltpu.get_barrier_semaphore()

    @pl.loop(1, n)
    def _(j):
        pl.semaphore_signal(barrier, inc=1, device_id=(xor_of(me, j, n), tp),
                               device_id_type=pl.DeviceIdType.MESH)

    for peer in (mate, across):
        pl.semaphore_signal(barrier, inc=1, device_id=(me, peer),
                               device_id_type=pl.DeviceIdType.MESH)
    pl.semaphore_wait(barrier, n + 1)

    @pl.loop(1, n)
    def _(j):
        sp_copy(j).start()

    for load in loads:
        load.start()

    def compute(s):
        x = rows[s]
        gate = jnp.dot(x, wg[...], preferred_element_type=jnp.float32)
        upper = jnp.dot(x, wu[...], preferred_element_type=jnp.float32)
        hidden = (gate * (1.0 / (1.0 + jnp.exp(-gate))) * upper).astype(jnp.bfloat16)
        width = wd.shape[1]
        tile = min(1024, width)

        @pl.loop(0, width // tile)
        def _(k):
            cols = pl.ds(pl.multiple_of(k * tile, tile), tile)
            parts[s, :, cols] = jnp.dot(
                hidden, wd[:, cols], preferred_element_type=jnp.float32
            ).astype(jnp.bfloat16)

    @pl.loop(0, n + 3)
    def _(j):
        @pl.when(j == 0)
        def _():
            own.wait()

        @pl.when((j >= 1) & (j < n))
        def _():
            sp_copy(j).wait_recv()

        @pl.when(j < n)
        def _():
            fy_copy(j).start()
            fa_copy(j).start()

        @pl.when((j >= 2) & (j < n + 2))
        def _():
            k = j - 2
            s = chunk(k)
            pp_copy(k).wait_recv()
            there = spot(core, 1 - y)
            far = pl.ds(pl.multiple_of((1 - y) * C, C), C)
            parts[s, there] = (
                parts[s, there].astype(jnp.float32) + pair_in[s, far].astype(jnp.float32)
            ).astype(jnp.bfloat16)
            ry_copy(k).start()

        @pl.when(j >= 3)
        def _():
            k = j - 3
            s = chunk(k)
            ry_copy(k).wait_recv()
            here = spot(core, y)
            near = pl.ds(pl.multiple_of(y * C, C), C)
            total = (
                parts[s, here].astype(jnp.float32)
                + pair_in[s, near].astype(jnp.float32)
                + y_in[s].astype(jnp.float32)
            ).astype(jnp.bfloat16)

            @pl.when(k == 0)
            def _():
                out[me] = total

            @pl.when(k > 0)
            def _():
                parts[s, here] = total
                rs_copy(k).start()

        @pl.when((j >= 1) & (j < n + 1))
        def _():
            k = j - 1
            fy_copy(k).wait_recv()
            fb_copy(k).start()

            @pl.when(k == 0)
            def _():
                for load in loads:
                    load.wait()

            fa_copy(k).wait_recv()
            fb_copy(k).wait_recv()
            compute(chunk(k))
            pp_copy(k).start()

    @pl.loop(0, n)
    def _(j):
        fy_copy(j).wait_send()
        fa_copy(j).wait_send()
        fb_copy(j).wait_send()
        pp_copy(j).wait_send()
        ry_copy(j).wait_send()

        @pl.when(j > 0)
        def _():
            sp_copy(j).wait_send()
            rs_copy(j).wait_send()
            rs_copy(j).wait_recv()


def moe_exchange(outgoing, w_gate, w_up, w_down, slices):
    n, capacity, width = outgoing.shape
    units = w_gate.shape[2]
    bf16 = jnp.bfloat16
    dma = pltpu.SemaphoreType.DMA
    return pl.pallas_call(
        functools.partial(moe_kernel, n, slices, capacity),
        out_shape=jax.ShapeDtypeStruct(outgoing.shape, bf16),
        in_specs=[pl.BlockSpec(memory_space=pltpu.VMEM)]
        + [pl.BlockSpec(memory_space=pl.ANY)] * 3,
        out_specs=pl.BlockSpec(memory_space=pltpu.VMEM),
        scratch_shapes=[
            pltpu.VMEM((width, units), bf16),
            pltpu.VMEM((width, units), bf16),
            pltpu.VMEM((units, width), bf16),
            pltpu.VMEM((n, slices * capacity, width), bf16),
            pltpu.VMEM((n, slices * capacity, width), bf16),
            pltpu.VMEM((n, 2 * capacity, width), bf16),
            pltpu.VMEM((n, capacity, width), bf16),
            dma((3,)),
            dma,
        ]
        + [dma((n,))] * 14,
        compiler_params=pltpu.CompilerParams(
            collective_id=1, has_side_effects=True, vmem_limit_bytes=52 * 2**20
        ),
        cost_estimate=pl.CostEstimate(
            flops=6 * n * slices * capacity * width * units,
            bytes_accessed=3 * 2 * width * units,
            transcendentals=0,
        ),
        name="moe_exchange",
    )(outgoing, w_gate, w_up, w_down)


def sum_kernel(count, part, out, pair_in, total, y_in, pp_send, pp_recv, y_send, y_recv):
    me = lax.axis_index("sp")
    tp = lax.axis_index("tp")
    core, y = tp % 2, tp // 2
    mate = y * 2 + (1 - core)
    across = (1 - y) * 2 + core
    pieces = count // 16
    mesh_id = pl.DeviceIdType.MESH
    barrier = pltpu.get_barrier_semaphore()
    for peer in (mate, across):
        pl.semaphore_signal(barrier, inc=1, device_id=(me, peer), device_id_type=mesh_id)
    pl.semaphore_wait(barrier, 2)

    def at(yy, c, k):
        return pl.ds(pl.multiple_of((yy * 2 + c) * count + k * 16, 16), 16)

    def piece(k):
        return pl.ds(pl.multiple_of(k * 16, 16), 16)

    def pair_copy(yy, k, place):
        return pltpu.make_async_remote_copy(
            src_ref=part.at[at(yy, 1 - core, k)], dst_ref=pair_in.at[place, piece(k)],
            send_sem=pp_send.at[place, k], recv_sem=pp_recv.at[place, k],
            device_id=(me, mate), device_id_type=mesh_id,
        )

    def far_copy(k):
        return pltpu.make_async_remote_copy(
            src_ref=total.at[piece(k)], dst_ref=y_in.at[piece(k)],
            send_sem=y_send.at[k], recv_sem=y_recv.at[k],
            device_id=(me, across), device_id_type=mesh_id,
        )

    @pl.loop(0, pieces)
    def _(k):
        pair_copy(1 - y, k, 0).start()

    @pl.loop(0, pieces)
    def _(k):
        pair_copy(y, k, 1).start()

    @pl.loop(0, pieces)
    def _(k):
        pair_copy(1 - y, k, 0).wait_recv()
        total[piece(k)] = (
            part[at(1 - y, core, k)].astype(jnp.float32)
            + pair_in[0, piece(k)].astype(jnp.float32)
        ).astype(jnp.bfloat16)
        far_copy(k).start()

    @pl.loop(0, pieces)
    def _(k):
        pair_copy(y, k, 1).wait_recv()
        far_copy(k).wait_recv()
        out[piece(k)] = (
            part[at(y, core, k)].astype(jnp.float32)
            + pair_in[1, piece(k)].astype(jnp.float32)
            + y_in[piece(k)].astype(jnp.float32)
        ).astype(jnp.bfloat16)

    @pl.loop(0, pieces)
    def _(k):
        pair_copy(1 - y, k, 0).wait_send()
        pair_copy(y, k, 1).wait_send()
        far_copy(k).wait_send()


def scatter_sum(part, slices):
    row_count, width = part.shape
    count = row_count // slices
    pieces = count // 16
    bf16 = jnp.bfloat16
    dma = pltpu.SemaphoreType.DMA
    return pl.pallas_call(
        functools.partial(sum_kernel, count),
        out_shape=jax.ShapeDtypeStruct((count, width), bf16),
        in_specs=[pl.BlockSpec(memory_space=pltpu.VMEM)],
        out_specs=pl.BlockSpec(memory_space=pltpu.VMEM),
        scratch_shapes=[
            pltpu.VMEM((2, count, width), bf16),
            pltpu.VMEM((count, width), bf16),
            pltpu.VMEM((count, width), bf16),
            dma((2, pieces)),
            dma((2, pieces)),
            dma((pieces,)),
            dma((pieces,)),
        ],
        compiler_params=pltpu.CompilerParams(
            collective_id=2, has_side_effects=True, vmem_limit_bytes=24 * 2**20
        ),
        cost_estimate=pl.CostEstimate(flops=0, bytes_accessed=2**25, transcendentals=0),
        name="scatter_sum",
    )(part)


def on_device(
    resid,
    pool_in,
    pool_mix,
    pool_gain,
    out_proj,
    norm_gain,
    w_gate,
    w_up,
    w_down,
    routes,
    route_weight,
):
    token_count, width = resid.shape
    choose = routes.shape[1]
    experts = lax.axis_size("sp")
    slices = lax.axis_size("tp")
    sub_count = token_count // slices
    capacity = max(2, 2 * sub_count * choose // experts)
    tp_index = lax.axis_index("tp")
    diff = group_diff(pool_in)
    pooled = (jnp.dot(diff, pool_mix[0], preferred_element_type=jnp.float32) * pool_gain).astype(
        jnp.bfloat16
    )
    group_part = rounded(jnp.dot(pooled, out_proj, preferred_element_type=jnp.float32)).astype(
        jnp.bfloat16
    )
    if slices == 4 and sub_count % 16 == 0:
        proj = scatter_sum(group_part, slices).astype(jnp.float32)
    else:
        proj = rounded(
            lax.psum_scatter(group_part, "tp", scatter_dimension=0, tiled=True).astype(jnp.float32)
        )
    first = tp_index * sub_count
    mixed = lax.dynamic_slice_in_dim(resid, first, sub_count, 0).astype(jnp.float32) + proj
    normed = normalize(mixed, norm_gain)
    route_rows = lax.dynamic_slice_in_dim(routes, first, sub_count, 0)
    weight_rows = lax.dynamic_slice_in_dim(route_weight, first, sub_count, 0)
    targets = slot_plan(route_rows, 1, capacity, experts)
    outgoing = fill_slots(normed, targets, experts * capacity).reshape(experts, capacity, width)
    if slices == 4 and capacity % 16 == 0 and experts & (experts - 1) == 0:
        returned = moe_exchange(outgoing, w_gate, w_up, w_down, slices)
    else:
        arrived = lax.all_to_all(outgoing, "sp", split_axis=0, concat_axis=0, tiled=True)
        block_rows = lax.all_gather(arrived, "tp", axis=0, tiled=True)
        spread = expert_part(block_rows.reshape(-1, width), w_gate, w_up, w_down).reshape(
            block_rows.shape
        )
        stacked = spread.reshape((slices,) + arrived.shape)
        received = lax.all_to_all(stacked, "tp", split_axis=0, concat_axis=0, tiled=True)
        summed = jnp.sum(received.astype(jnp.float32), axis=0)
        returned = lax.all_to_all(
            summed.astype(jnp.bfloat16), "sp", split_axis=0, concat_axis=0, tiled=True
        )
    moe = collect(returned.reshape(-1, width), targets, weight_rows)
    return (mixed + moe).astype(jnp.bfloat16)


def solution(mesh):
    in_specs = (
        P("sp", None),
        P("sp", "tp"),
        P("tp", None, None),
        P("tp"),
        P("tp", None),
        P(),
        P("sp", None, "tp"),
        P("sp", None, "tp"),
        P("sp", "tp", None),
        P("sp", None),
        P("sp", None),
    )
    out_specs = P(("sp", "tp"), None)
    return jax.shard_map(
        on_device, mesh=mesh, in_specs=in_specs, out_specs=out_specs, check_vma=False
    )
```
